32 devices in a mesh: sp: 8 (over z, y), tp: 4 (over x, core).
Axes of the slice: x: 2, y: 2, z: 4, core: 2. Of those that a mesh axis runs over, the one named last changes fastest.
Arguments:
- resid: bfloat16 [6144, 2048], P(('sp', 'tp')), may hold values from -6 to 6
- query: bfloat16 [6144, 1024], P('sp', 'tp'), may hold values from -6 to 6
- keys: bfloat16 [6144, 1024], P('sp', 'tp'), may hold values from -6 to 6
- values: bfloat16 [6144, 1024], P('sp', 'tp'), may hold values from -6 to 6
- out_gate: bfloat16 [6144, 1024], P(('sp', 'tp')), may hold values from -6 to 6
- forget_pre: float32 [4, 6144], P('tp', 'sp'), may hold values from 0 to 16
- input_pre: float32 [4, 6144], P('tp', 'sp'), may hold values from -4 to 130
- head_gain: float32 [1024], replicated, may hold values from 0.1 to 1.9
- out_proj: bfloat16 [1024, 2048], replicated, may hold values from -0.1875 to 0.1875
- ffn_gain: float32 [2048], replicated, may hold values from 0.1 to 1.9
- routes: int32 [6144, 2], P(('sp', 'tp')), may hold values from 0 to 7, all different within a row; in each aligned block of 96 rows (0 to 95, 96 to 191, ...) at most 48 rows name the same one
- route_scores: float32 [6144, 2], P(('sp', 'tp')), may hold values from 0.1 to 1
- w_gate: bfloat16 [8, 2048, 512], P('sp'), may hold values from -0.125 to 0.125
- w_up: bfloat16 [8, 2048, 512], P('sp'), may hold values from -0.125 to 0.125
- w_down: bfloat16 [8, 512, 2048], P('sp'), may hold values from -0.25 to 0.25
Outputs:
- layer_out: bfloat16 [6144, 2048], P(('sp', 'tp'))
The draws below stay inside these ranges and needn't reach their ends.
Inputs may be any that keep to these rules, and one draw needn't show every extreme that they name: `routes`: each row names 2 different experts; in each aligned block of 96 rows no expert is named by more than 48 rows, a bound that some block reaches.
All inputs are finite; a program needn't handle non-finite values.
Results may differ from the reference program's by a relative error of at most 0.0095.
Values may be sent and summed in bfloat16 or wider, within the bound.
No kernel may reach another device: no remote copies, remote signals or barrier semaphores. Data moves between devices by JAX's collectives and lax.ppermute only.
A program may use at most 128 MiB of HBM per device.

```python
import math
import jax
import jax.numpy as jnp
import numpy as np
from jax import lax

D = 2048
CELL_HEADS = 4
HEAD_DIM = 256
MDIM = 1024
FF = 512
EXPERTS = 8
TOPK = 2
BLOCK = 64
TOK_DEV = 768
SEQUENCE_TOKENS = 6144
HALF = 96
CAP = 48


def draw_forget_pre(key, part):
    split_random_keys = jax.random.split(jax.random.fold_in(key, 17), 5)
    head_order = jax.random.permutation(split_random_keys[0], CELL_HEADS)
    fast_heads = head_order < CELL_HEADS // 2
    jitter = jnp.clip(jax.random.normal(split_random_keys[1], (CELL_HEADS, SEQUENCE_TOKENS), jnp.float32) * 0.7, -2.4, 2.4)
    base_level = jnp.where(fast_heads, jnp.log(100.0), jnp.log(1.0 * SEQUENCE_TOKENS) + 1.5).astype(jnp.float32)
    factor = jax.random.uniform(split_random_keys[2], (SEQUENCE_TOKENS // TOK_DEV,), jnp.float32, 0.0, jnp.log(4.0))
    slow_part = jnp.repeat(factor, TOK_DEV, total_repeat_length=SEQUENCE_TOKENS)
    output_values = base_level[:, None] - slow_part[None, :] + jitter
    outlier_position = jax.random.randint(split_random_keys[3], (3,), 0, SEQUENCE_TOKENS)
    outlier_mask = jnp.any(jnp.arange(SEQUENCE_TOKENS)[:, None] == outlier_position[None, :], axis=1)
    outlier_value = jax.random.uniform(split_random_keys[4], (CELL_HEADS, SEQUENCE_TOKENS), jnp.float32, 0.0, 1.39)
    return jnp.where(outlier_mask[None, :], outlier_value, output_values)


def draw_input_pre(key, part):
    split_random_keys = jax.random.split(jax.random.fold_in(key, 29), 1)
    return jnp.clip(jax.random.normal(split_random_keys[0], (CELL_HEADS, SEQUENCE_TOKENS), jnp.float32), -4.0, 4.0)


def block_levels(stream_key, dims, pieces, least, largest):
    factor_of = 1.0
    for position, parts in pieces:
        steps = jax.random.uniform(jax.random.fold_in(jax.random.fold_in(stream_key, 6), position), (parts,), jnp.float32, least / len(pieces), largest / len(pieces))
        factor_of = factor_of * jnp.repeat(jnp.exp(steps), dims[position] // parts).reshape((-1,) + (1,) * (len(dims) - 1 - position))
    return factor_of


def shared_out(rng, own, number, rows, count, top, reach, skew):
    sequence = jax.random.permutation(rng, count)
    packed, ordinary = shares(count, rows * top, reach, skew, True), shares(count, rows * top, reach, skew, False)
    places = jnp.arange(count)

    def named(sizes, rotation):
        used = int((sizes > 0).sum())
        fixed = max(1, used // 4)
        moved = fixed + (places - fixed + rotation * (used - fixed)) % max(1, count - fixed)
        return jnp.zeros((count,), jnp.int32).at[sequence[jnp.where(places < fixed, places, moved)]].set(jnp.asarray(sizes, jnp.int32))

    sizes = jnp.where(number % 4 == 0, named(packed, number // 4), named(ordinary, number - number // 4 - 1))
    mixed = jax.random.permutation(jax.random.fold_in(own, 3), count)
    donor, sink = mixed[0:count // 2 * 2:2], mixed[1:count // 2 * 2:2]
    margin = jnp.minimum(sizes[donor] - 1, reach - sizes[sink]) // 2
    margin = jnp.where((donor == sequence[0]) | (sink == sequence[0]) | (sizes[sink] == 0), 0, jnp.maximum(margin, 0))
    moved = jax.random.randint(jax.random.fold_in(own, 4), (count // 2,), 0, 1 << 20) % (margin + 1)
    sizes = sizes.at[donor].add(-moved).at[sink].add(moved)
    labels = jnp.searchsorted(jnp.cumsum(sizes), jnp.arange(rows * top), side="right").astype(jnp.int32)
    grid = labels.reshape(top, rows).T
    grid = grid[jax.random.permutation(jax.random.fold_in(own, 1), rows)]
    rotation = jax.random.randint(jax.random.fold_in(own, 2), (rows, 1), 0, top)
    return jnp.take_along_axis(grid, (jnp.arange(top)[None, :] + rotation) % top, axis=1)


def shares(count, total, limit, skew, full):
    loads = [(1 << 20) // math.isqrt(rank ** skew) + 1 for rank in range(1, count + 1)]
    largest = limit if full else min(limit, max(-(-total // count), total * loads[0] // sum(loads)))
    least = 1 if total - largest >= count - 1 else 0
    counts, spare = [largest] + [least] * (count - 1), total - largest - least * (count - 1)
    while spare > 0:
        movable = [i for i in range(1, count) if counts[i] < largest] or [i for i in range(1, count) if counts[i] < limit]
        pool, left = sum([loads[i] for i in movable]), spare
        for i in movable:
            addition = min(limit - counts[i], max(1, left * loads[i] // pool), spare)
            counts[i] = counts[i] + addition
            spare = spare - addition
    return np.array(counts)


def centred(key, extent, spread, limit, shards=(), held_as=jnp.bfloat16):
    values = spread * jax.random.normal(key, extent, jnp.float32)
    if shards:
        values = values * block_levels(key, extent, shards, -0.22, 0.18)
    return jnp.clip(values, -limit, limit).astype(held_as)


def setup_inputs(seed: int = 0) -> dict:
    key_list = jax.random.split(jax.random.key(seed), 16)
    resid = centred(key_list[0], (SEQUENCE_TOKENS, D), 1.0, 6.0, ((0, 32),))
    query = centred(key_list[1], (SEQUENCE_TOKENS, MDIM), 1.0, 6.0, ((0, 8), (1, 4)))
    keys = centred(key_list[2], (SEQUENCE_TOKENS, MDIM), 1.0, 6.0, ((0, 8), (1, 4)))
    values = centred(key_list[3], (SEQUENCE_TOKENS, MDIM), 1.0, 6.0, ((0, 8), (1, 4)))
    out_gate = centred(key_list[4], (SEQUENCE_TOKENS, MDIM), 1.0, 6.0, ((0, 32),))
    forget_pre = draw_forget_pre(jax.random.fold_in(key_list[15], 71), 0)
    input_pre = draw_input_pre(jax.random.fold_in(key_list[15], 71), 0)
    head_gain = jnp.clip(1.0 + 0.18 * jax.random.normal(key_list[7], (MDIM,), jnp.float32), 0.1, 1.9)
    out_proj = centred(key_list[8], (MDIM, D), MDIM ** -0.5, 0.1875)
    ffn_gain = jnp.clip(1.0 + 0.18 * jax.random.normal(key_list[9], (D,), jnp.float32), 0.1, 1.9)
    routes_keys = jax.random.split(jax.random.fold_in(key_list[10], 1), SEQUENCE_TOKENS // HALF)
    routes_turns = jax.random.permutation(jax.random.fold_in(key_list[10], 3), SEQUENCE_TOKENS // HALF)
    routes = jax.vmap(lambda own, number: shared_out(jax.random.fold_in(key_list[10], 2), own, number, HALF, EXPERTS, TOPK, CAP, 1))(routes_keys, routes_turns).reshape((SEQUENCE_TOKENS, TOPK))
    route_scores = jnp.clip(0.1 + 0.9 * jax.random.uniform(key_list[11], (SEQUENCE_TOKENS, TOPK), jnp.float32) ** block_levels(key_list[11], (SEQUENCE_TOKENS, TOPK), ((0, 32),), -0.2, 0.2), 0.1, 1.0)
    w_gate = centred(key_list[12], (EXPERTS, D, FF), D ** -0.5, 0.125, ((0, 8),))
    w_up = centred(key_list[13], (EXPERTS, D, FF), D ** -0.5, 0.125, ((0, 8),))
    w_down = centred(key_list[14], (EXPERTS, FF, D), FF ** -0.5, 0.25, ((0, 8),))
    return {"resid": resid, "query": query, "keys": keys, "values": values, "out_gate": out_gate, "forget_pre": forget_pre, "input_pre": input_pre, "head_gain": head_gain, "out_proj": out_proj, "ffn_gain": ffn_gain, "routes": routes, "route_scores": route_scores, "w_gate": w_gate, "w_up": w_up, "w_down": w_down}


EPS = 1e-06
HIGHEST = lax.Precision.HIGHEST

def block_pass(query, keys, values, log_forget, log_input, state):
    seq_len, head_width = query.shape
    blocks = seq_len // BLOCK
    key_scale = head_width ** (-0.5)
    causal = jnp.tril(jnp.ones((BLOCK, BLOCK), dtype=bool))

    def block_step(state_in, inputs):
        state_mat, state_vec, max_log = state_in
        q_block, k_block, v_block, forget_blk, input_blk = inputs
        cum_log = jnp.cumsum(forget_blk)
        block_total = cum_log[-1]
        log_mat = jnp.where(causal, cum_log[:, None] - cum_log[None, :] + input_blk[None, :], -jnp.inf)
        inter_log = cum_log + max_log
        row_max = jnp.maximum(inter_log, lax.optimization_barrier(jnp.max(log_mat, axis=1)))
        weight_mat = jnp.exp(log_mat - row_max[:, None])
        carry_weight = jnp.exp(inter_log - row_max)
        scores = jnp.dot(q_block, k_block.T, preferred_element_type=jnp.float32) * key_scale
        weights_blk = (scores * weight_mat).astype(jnp.bfloat16)
        q_float = q_block.astype(jnp.float32)
        numerator = carry_weight[:, None] * jnp.dot(q_float, state_mat, precision=HIGHEST) + jnp.dot(weights_blk, v_block, preferred_element_type=jnp.float32)
        denominator = carry_weight * jnp.dot(q_float, state_vec, precision=HIGHEST) + lax.optimization_barrier(jnp.sum(weights_blk.astype(jnp.float32), axis=1))
        log_keep = block_total - cum_log + input_blk
        new_max = jnp.maximum(block_total + max_log, jnp.max(log_keep))
        keep_weight = jnp.exp(log_keep - new_max)
        decay_now = jnp.exp(block_total + max_log - new_max)
        k_float = k_block.astype(jnp.float32) * key_scale
        state_mat = decay_now * state_mat + jnp.dot((k_float * keep_weight[:, None]).T, v_block.astype(jnp.float32), precision=HIGHEST)
        state_vec = decay_now * state_vec + jnp.dot(keep_weight, k_float, precision=HIGHEST)
        return ((state_mat, state_vec, new_max), (numerator, denominator, row_max))

    def to_blocks(array_in):
        return array_in.reshape((blocks, BLOCK) + array_in.shape[1:])
    ignored, outputs = lax.scan(block_step, state, (to_blocks(query), to_blocks(keys), to_blocks(values), to_blocks(log_forget), to_blocks(log_input)))
    numerator, denominator, row_max = outputs
    return (numerator.reshape(seq_len, head_width), denominator.reshape(seq_len), row_max.reshape(seq_len))

def reference(resid, query, keys, values, out_gate, forget_pre, input_pre, head_gain, out_proj, ffn_gain, routes, route_scores, w_gate, w_up, w_down):
    log_forget = jax.nn.log_sigmoid(forget_pre)
    start_state = (jnp.zeros((HEAD_DIM, HEAD_DIM), jnp.float32), jnp.zeros((HEAD_DIM,), jnp.float32), jnp.zeros((), jnp.float32))
    head_outs = []
    for head_idx in range(CELL_HEADS):
        col_start = head_idx * HEAD_DIM
        col_end = col_start + HEAD_DIM
        numerator, denominator, row_max = block_pass(query[:, col_start:col_end], keys[:, col_start:col_end], values[:, col_start:col_end], log_forget[head_idx], input_pre[head_idx], start_state)
        hidden = numerator / jnp.maximum(jnp.abs(denominator), jnp.exp(-row_max))[:, None]
        head_outs.append(hidden)
    cell_rows = lax.optimization_barrier(jnp.concatenate(head_outs, axis=1).astype(jnp.bfloat16))
    cell_float = cell_rows.astype(jnp.float32)
    headed = cell_float * lax.rsqrt(lax.optimization_barrier(jnp.mean(cell_float * cell_float, axis=1, keepdims=True)) + EPS) * head_gain[None, :]
    gated_out = (headed * jax.nn.sigmoid(out_gate.astype(jnp.float32))).astype(jnp.bfloat16)
    after_mix = resid.astype(jnp.float32) + jnp.dot(gated_out, out_proj, preferred_element_type=jnp.float32)
    normed_rows = (after_mix * lax.rsqrt(lax.optimization_barrier(jnp.mean(after_mix * after_mix, axis=1, keepdims=True)) + EPS) * ffn_gain[None, :]).astype(jnp.bfloat16)
    flat_ids = routes.reshape(-1).astype(jnp.int32)
    one_hot = (flat_ids[:, None] == jnp.arange(EXPERTS, dtype=jnp.int32)[None, :]).astype(jnp.int32)
    slot_rank = lax.optimization_barrier(jnp.sum((jnp.cumsum(one_hot, axis=0) - 1) * one_hot, axis=1)).astype(jnp.int32)
    most_rows = SEQUENCE_TOKENS // HALF * CAP
    index_table = jnp.zeros((EXPERTS, most_rows), jnp.int32).at[flat_ids, slot_rank].set(jnp.arange(flat_ids.shape[0], dtype=jnp.int32) // TOPK)

    def one_expert(operands):
        row_picks, gate_mat, up_mat, down_mat = operands
        tok_rows = normed_rows[row_picks]
        gate_pre = jnp.dot(tok_rows, gate_mat, preferred_element_type=jnp.float32)
        up_pre = jnp.dot(tok_rows, up_mat, preferred_element_type=jnp.float32)
        active = (jax.nn.silu(gate_pre) * up_pre).astype(jnp.bfloat16)
        return jnp.dot(active, down_mat, preferred_element_type=jnp.float32).astype(jnp.bfloat16)
    expert_out = lax.map(one_expert, (index_table, w_gate, w_up, w_down))
    assigned = expert_out[flat_ids, slot_rank].astype(jnp.float32).reshape(SEQUENCE_TOKENS, TOPK, D)
    route_weight = route_scores / lax.optimization_barrier(jnp.sum(route_scores, axis=1, keepdims=True))
    combined = lax.optimization_barrier(jnp.sum(assigned * route_weight[:, :, None], axis=1))
    return (after_mix + combined).astype(jnp.bfloat16)
```

```python
import functools
import math

import jax
import jax.numpy as jnp
from jax import lax
from jax.experimental import pallas as pl
from jax.experimental.pallas import tpu as pltpu
from jax.sharding import PartitionSpec as P


BLOCK = 64
EPS = 1e-06
FLOOR_LOG = -1e30
AUX_ROWS = 8


def dot(a, b, contract):
    return lax.dot_general(a, b, (contract, ((), ())), preferred_element_type=jnp.float32)


def iota(shape, axis):
    return lax.broadcasted_iota(jnp.int32, shape, axis)


def split_three(x):
    first = x.astype(jnp.bfloat16)
    rest = x - first.astype(jnp.float32)
    second = rest.astype(jnp.bfloat16)
    third = (rest - second.astype(jnp.float32)).astype(jnp.bfloat16)
    return first, second, third


def split_two(x):
    first = x.astype(jnp.bfloat16)
    return first, (x - first.astype(jnp.float32)).astype(jnp.bfloat16)


def pick_rows(rows, count, width):
    row = iota((count, width), 0)
    out = jnp.zeros((count, width), jnp.float32)
    for index, value in enumerate(rows):
        out = jnp.where(row == index, value, out)
    return out


def to_column(row, size):
    eye = iota((size, size), 0) == iota((size, size), 1)
    return jnp.sum(jnp.where(eye, row, 0.0), axis=1, keepdims=True)


def pack_aux(vec, top, total, width):
    return pick_rows([vec, top, total, jnp.ones((1, 1), jnp.float32)], AUX_ROWS, width)


def unpack_aux(aux):
    valid = aux[3:4] > 0.5
    return aux[0:1], jnp.where(valid, aux[1:2], FLOOR_LOG)[:, :1], aux[2:3, :1]


def state_kernel(k_ref, v_ref, forget_ref, input_ref, send_ref, mat_ref, aux_ref, gates_ref, *, chunk):
    seq_len, width = k_ref.shape
    pre = jnp.broadcast_to(forget_ref[...], (8, seq_len))
    log_forget = jnp.minimum(pre, 0.0) - jnp.log1p(jnp.exp(-jnp.abs(pre)))
    cum = jnp.zeros((8, seq_len), jnp.float32)
    upper = (iota((seq_len, seq_len), 0) <= iota((seq_len, seq_len), 1)).astype(jnp.bfloat16)
    for part in reversed(split_three(log_forget)):
        cum = cum + dot(part, upper, ((1,), (0,)))
    level = input_ref[...] - cum
    gates_ref[...] = jnp.where(iota((8, seq_len), 0) == 0, level, cum)
    top = jnp.max(level[:1], axis=1, keepdims=True)
    total = jnp.sum(jnp.where(iota((1, seq_len), 1) == seq_len - 1, cum[:1], 0.0), axis=1, keepdims=True)
    weight = jnp.exp(level[:1] - top)
    mat = jnp.zeros((width, width), jnp.float32)
    vec = jnp.zeros((1, width), jnp.float32)
    for start in range(0, seq_len, chunk):
        here = slice(start, start + chunk)
        column = to_column(weight[:, here], chunk) * width ** (-0.5)
        scaled = k_ref[here, :].astype(jnp.float32) * column
        for part in split_two(scaled):
            vec = vec + jnp.sum(part.astype(jnp.float32), axis=0, keepdims=True)
            mat = mat + dot(part, v_ref[here, :], ((0,), (0,)))
    last = top + total
    mat_ref[...] = mat
    aux_ref[...] = pick_rows([vec, last, total], 8, width)
    send_ref[:width, :] = mat
    send_ref[width:, :] = pack_aux(vec, last, total, width)


def local_kernel(q_ref, k_ref, v_ref, gates_ref, num_ref, stat_ref, *, chunk):
    seq_len, width = q_ref.shape
    key_scale = width ** (-0.5)
    for start in range(0, seq_len, chunk):
        end = start + chunk
        here = slice(start, end)
        scores = dot(q_ref[here, :], k_ref[:end, :], ((1,), (1,))) * key_scale
        row = iota((chunk, end), 0) + start
        col = iota((chunk, end), 1)
        level = jnp.where(col <= row, gates_ref[0:1, :end], -jnp.inf)
        top = jnp.max(level, axis=1, keepdims=True)
        weight = scores * jnp.exp(level - top)
        first = weight.astype(jnp.bfloat16)
        rest = weight - first.astype(jnp.float32)
        own_block = col >= (row // BLOCK) * BLOCK
        second = jnp.where(own_block, 0.0, rest).astype(jnp.bfloat16)
        num_ref[here, :] = dot(first, v_ref[:end, :], ((1,), (0,))) + dot(
            second, v_ref[:end, :], ((1,), (0,))
        )
        den = jnp.sum(first.astype(jnp.float32) + second.astype(jnp.float32), axis=1, keepdims=True)
        cum = to_column(gates_ref[1:2, here], chunk)
        lane = iota((chunk, 128), 1)
        stat_ref[here, :] = jnp.where(lane == 0, den, jnp.where(lane == 1, top, cum))


def merge(old, new):
    old_mat, old_vec, old_max, old_total = old
    new_mat, new_vec, new_max, new_total = new
    joined = jnp.maximum(new_total + old_max, new_max)
    keep_old = jnp.exp(new_total + old_max - joined)
    keep_new = jnp.exp(new_max - joined)
    return (
        keep_old * old_mat + keep_new * new_mat,
        keep_old * old_vec + keep_new * new_vec,
        joined,
        old_total + new_total,
    )


def read_state(mat_ref, aux_ref):
    return (mat_ref[...], aux_ref[0:1, :], aux_ref[1:2, :1], aux_ref[2:3, :1])


def write_state(state, mat_ref, aux_ref):
    mat_ref[...] = state[0]
    aux_ref[...] = pick_rows(state[1:], 8, state[0].shape[1])


def join_kernel(got_ref, mat_ref, aux_ref, far_mat_ref, far_aux_ref, send_ref, mat_out, aux_out, far_mat_out, far_aux_out):
    width = mat_ref.shape[0]
    got = (got_ref[:width, :],) + unpack_aux(got_ref[width:, :])
    state = merge(got, read_state(mat_ref, aux_ref))
    write_state(state, mat_out, aux_out)
    write_state(merge(got, read_state(far_mat_ref, far_aux_ref)), far_mat_out, far_aux_out)
    send_ref[:width, :] = state[0]
    send_ref[width:, :] = pack_aux(*state[1:], width)


def masked(state, valid):
    mat, vec, top, total = state
    return (
        jnp.where(valid, mat, 0.0),
        jnp.where(valid, vec, 0.0),
        jnp.where(valid, top, FLOOR_LOG),
        jnp.where(valid, total, 0.0),
    )


def read_sent(ref):
    width = ref.shape[1]
    return (ref[:width, :],) + unpack_aux(ref[width:, :])


def pair_kernel(place_ref, got_ref, mat_ref, aux_ref, send_ref):
    width = mat_ref.shape[0]
    odd = place_ref[0] % 2 == 1
    own, other = read_state(mat_ref, aux_ref), read_sent(got_ref)
    early = [jnp.where(odd, b, a) for a, b in zip(own, other)]
    late = [jnp.where(odd, a, b) for a, b in zip(own, other)]
    state = merge(early, late)
    send_ref[:width, :] = state[0]
    send_ref[width:, :] = pack_aux(*state[1:], width)


def read_out(far, q_ref, num_ref, stat_ref, out_ref, chunk):
    mat, vec, far_max, _ = far
    mats = split_three(mat)
    for start in range(0, q_ref.shape[0], chunk):
        here = slice(start, start + chunk)
        query = q_ref[here, :]
        den, top, cum = (stat_ref[here, index : index + 1] for index in range(3))
        joined = jnp.maximum(top, far_max)
        keep_own = jnp.exp(top - joined)
        keep_far = jnp.exp(far_max - joined)
        far_num = sum(dot(query, part, ((1,), (0,))) for part in reversed(mats))
        far_den = jnp.sum(query.astype(jnp.float32) * vec, axis=1, keepdims=True)
        num = keep_own * num_ref[here, :] + keep_far * far_num
        den = keep_own * den + keep_far * far_den
        floor = jnp.exp(-(cum + joined))
        out_ref[here, :] = (num / jnp.maximum(jnp.abs(den), floor)).astype(jnp.bfloat16)


def finish_kernel(got_ref, far_mat_ref, far_aux_ref, q_ref, num_ref, stat_ref, out_ref, *, chunk):
    far = merge(read_sent(got_ref), read_state(far_mat_ref, far_aux_ref))
    read_out(far, q_ref, num_ref, stat_ref, out_ref, chunk)


def finish_pairs_kernel(place_ref, *refs, chunk, far_count):
    place = place_ref[0]
    width = refs[0].shape[1]
    far = (jnp.zeros((width, width), jnp.float32), jnp.zeros((1, width), jnp.float32))
    far += (jnp.full((1, 1), FLOOR_LOG, jnp.float32), jnp.zeros((1, 1), jnp.float32))
    for back in range(far_count, 0, -1):
        far = merge(far, masked(read_sent(refs[back]), place // 2 >= back))
    far = merge(far, masked(read_sent(refs[0]), place % 2 == 1))
    read_out(far, *refs[far_count + 1 :], chunk)


def call(kernel, outs, *args, specs=None, scratch=(), vmem=16, flops=0, **kwargs):
    extra = {} if specs is None else {"in_specs": specs}
    if flops:
        extra["cost_estimate"] = pl.CostEstimate(flops=flops, transcendentals=0, bytes_accessed=0)
    return pl.pallas_call(
        functools.partial(kernel, **kwargs),
        out_shape=[jax.ShapeDtypeStruct(shape, dtype) for shape, dtype in outs],
        scratch_shapes=scratch,
        compiler_params=pltpu.CompilerParams(vmem_limit_bytes=vmem * 2**20),
        **extra,
    )(*args)


SCALAR = pl.BlockSpec(memory_space=pltpu.SMEM)
VECTOR = pl.BlockSpec(memory_space=pltpu.VMEM)
REMOTE = pl.BlockSpec(memory_space=pltpu.HBM)
RING = 4
VMEM_SLOT = 36


def ring_shift(array, step=1):
    places = lax.axis_size("sp")
    return lax.ppermute(array, "sp", [(place, (place + 2 * step) % places) for place in range(places)])


def pair_swap(array):
    return lax.ppermute(array, "sp", [(place, place ^ 1) for place in range(lax.axis_size("sp"))])


def side_swap(array, distance):
    return lax.ppermute(array, "tp", [(place, place ^ distance) for place in range(lax.axis_size("tp"))])


def ring_fits():
    places = lax.axis_size("sp")
    return places == 2 * RING and lax.axis_size("tp") % 4 == 0


def cell_head(query, keys, values, forget_pre, input_pre):
    seq_len, width = query.shape
    chunk = math.gcd(seq_len, 128)
    f32, b16 = jnp.float32, jnp.bfloat16
    states = [((width, width), f32), ((8, width), f32)]
    sent = [((width + AUX_ROWS, width), f32)]
    send, mat, aux, gates = call(
        state_kernel,
        sent + states + [((8, seq_len), f32)],
        keys,
        values,
        forget_pre,
        input_pre,
        vmem=56,
        chunk=chunk,
    )
    num, stat = call(
        local_kernel, [((seq_len, width), f32), ((seq_len, 128), f32)], query, keys, values, gates, chunk=chunk
    )
    if ring_fits():
        place = lax.axis_index("sp").astype(jnp.int32).reshape(1)
        pair = pair_swap(send)
        slab = call(pair_kernel, sent, place, pair, mat, aux, specs=[SCALAR] + [VECTOR] * 3)[0]
        far_count = lax.axis_size("sp") // 2 - 1
        fars = []
        for back in range(far_count):
            fars.append(ring_shift(slab, back + 1))
        operands = [pair, *fars, query, num, stat]
        rows = call(
            finish_pairs_kernel,
            [((seq_len, width), b16)],
            place,
            *operands,
            specs=[SCALAR] + [VECTOR] * len(operands),
            chunk=chunk,
            far_count=far_count,
        )[0]
        return rows, (send, stat, fars, rows)
    far_mat = jnp.zeros((width, width), f32)
    far_aux = jnp.where(iota((8, width), 0) == 1, FLOOR_LOG, 0.0)
    places = lax.axis_size("sp")
    step = 1
    got = jnp.zeros(sent[0][0], f32)
    while step < places:
        got = lax.ppermute(send, "sp", [(place, place + step) for place in range(places - step)])
        step *= 2
        if step < places:
            send, mat, aux, far_mat, far_aux = call(
                join_kernel, sent + states + states, got, mat, aux, far_mat, far_aux
            )
    rows = call(
        finish_kernel, [((seq_len, width), b16)], got, far_mat, far_aux, query, num, stat, chunk=chunk
    )[0]
    return rows, got


def mix_kernel(rows_ref, gate_ref, gain_ref, proj_ref, resid_ref, ffn_gain_ref, mix_ref, norm_ref):
    rows = rows_ref[...].astype(jnp.float32)
    headed = rows * lax.rsqrt(jnp.mean(rows * rows, axis=1, keepdims=True) + EPS) * gain_ref[...]
    gated = (headed * jax.nn.sigmoid(gate_ref[...].astype(jnp.float32))).astype(jnp.bfloat16)
    mix = resid_ref[...].astype(jnp.float32) + dot(gated, proj_ref[...], ((1,), (0,)))
    mix_ref[...] = mix
    norm = mix * lax.rsqrt(jnp.mean(mix * mix, axis=1, keepdims=True) + EPS) * ffn_gain_ref[...]
    norm_ref[...] = norm.astype(jnp.bfloat16)


def gate_kernel(heads_ref, gate_ref, gain_ref, out_ref):
    count, _, width = heads_ref.shape
    heads = [heads_ref[head].astype(jnp.float32) for head in range(count)]
    squares = sum(jnp.sum(rows * rows, axis=1, keepdims=True) for rows in heads)
    scale = lax.rsqrt(squares / (count * width) + EPS)
    for head, rows in enumerate(heads):
        here = slice(head * width, (head + 1) * width)
        gate = jax.nn.sigmoid(gate_ref[:, here].astype(jnp.float32))
        out_ref[:, here] = (rows * scale * gain_ref[:, here] * gate).astype(jnp.bfloat16)


def route_kernel(routes_ref, scores_ref, out_ref, *, expert_count):
    scores = scores_ref[...]
    weight = scores / jnp.sum(scores, axis=0, keepdims=True)
    row = iota(out_ref.shape, 0)
    dense = jnp.zeros(out_ref.shape, jnp.float32)
    for route in range(scores.shape[0]):
        named = row % expert_count == routes_ref[route : route + 1, :]
        dense = dense + jnp.where(named, weight[route : route + 1, :], 0.0)
    first, second, third = (part.astype(jnp.float32) for part in split_three(dense))
    place = row // expert_count
    packed = jnp.where(place == 0, first, jnp.where(place == 1, second, third))
    out_ref[...] = jnp.where(place < 3, packed, 0.0).astype(jnp.bfloat16)


def expert_weight(route_ref, expert_count, expert):
    row = iota(route_ref.shape, 0)
    mine = (row % expert_count == expert) & (row < 3 * expert_count)
    weight = jnp.sum(jnp.where(mine, route_ref[...].astype(jnp.float32), 0.0), axis=0, keepdims=True)
    return to_column(weight, route_ref.shape[1])


def mix_rows(gated_ref, resid_ref, proj, gain_ref):
    mix = resid_ref[...].astype(jnp.float32) + dot(gated_ref[...], proj, ((1,), (0,)))
    norm = mix * lax.rsqrt(jnp.mean(mix * mix, axis=1, keepdims=True) + EPS) * gain_ref[...]
    return mix, norm.astype(jnp.bfloat16)


def own_mix_kernel(gated_ref, resid_ref, gain_ref, proj_ref, mix_ref, norm_ref):
    mix_ref[...], norm_ref[...] = mix_rows(gated_ref, resid_ref, proj_ref[...], gain_ref)


def slot_kernel(place_ref, route_ref, *refs, expert_count, given, count):
    lead, sources, out_ref = refs[:given], refs[given : given + count], refs[given + count]
    places, sems = refs[given + count + 1 : -1], refs[-1]
    solid = count - 12
    targets = list(places[:solid])
    _, part = sources[solid].shape
    for index in range(4):
        here = pl.ds(index * part, part)
        targets += [
            places[solid].at[:, here],
            places[solid + 1].at[:, here],
            places[solid + 2].at[here, :],
        ]
    copies = [
        pltpu.make_async_copy(source, target, sems.at[index])
        for index, (source, target) in enumerate(zip(sources, targets))
    ]
    order = list(range(solid))
    order += [solid + 3 * quarter + kind for kind in range(3) for quarter in range(4)]
    for index in order:
        copies[index].start()

    def ready(place):
        for index in [place] if place < solid else range(place, count, 3):
            copies[index].wait()
        return places[place][...]

    if solid == 4:
        gated_ref, resid_ref, gain_ref = lead
        _, rows = mix_rows(gated_ref, resid_ref, ready(0), gain_ref)
    else:
        rows = lead[0][...]

    def expert_part(first):
        gate = dot(rows, ready(first), ((1,), (0,)))
        up = dot(rows, ready(first + 1), ((1,), (0,)))
        active = (jax.nn.silu(gate) * up).astype(jnp.bfloat16)
        return dot(active, ready(first + 2), ((1,), (0,))).astype(jnp.bfloat16).astype(jnp.float32)

    place = place_ref[0]
    other = place + 1 - 2 * (place % 2)
    total = expert_part(solid - 3) * expert_weight(route_ref, expert_count, place)
    total = total + expert_part(solid) * expert_weight(route_ref, expert_count, other)
    if given == 2:
        total = total + lead[1][...]
    out_ref[...] = total.astype(out_ref.dtype)


def part_size(arrays):
    return sum(math.prod(array.shape) for array in arrays)


def ring_experts(lead_in, cell_parts, gated, ffn_gain, out_proj, w_gate, w_up, w_down):
    resid, routes, route_scores = lead_in
    places = lax.axis_size("sp")
    rows, width = resid.shape
    place = lax.axis_index("sp").astype(jnp.int32).reshape(1)
    names = -(-3 * places // 16) * 16
    routed = call(
        route_kernel, [((names, rows), jnp.bfloat16)], routes.T, route_scores.T, expert_count=places
    )[0]
    send, stat, fars, cell_rows = cell_parts
    part = w_gate.shape[2] // 4
    quarter = lax.axis_index("tp") % 4
    quarters = [
        lax.dynamic_slice_in_dim(w_gate[0], quarter * part, part, 1),
        lax.dynamic_slice_in_dim(w_up[0], quarter * part, part, 1),
        lax.dynamic_slice_in_dim(w_down[0], quarter * part, part, 0),
        lax.dynamic_slice_in_dim(w_down[0], (quarter ^ 2) * part, part, 0),
    ]
    quarters, _ = lax.optimization_barrier((quarters, send))
    near, cross, far = [], [], []
    for index in range(4):
        near.append(pair_swap(quarters[index]))
    for index, token in enumerate((stat, cell_rows)):
        source, _ = lax.optimization_barrier((near[index], token))
        cross.append(side_swap(source, 2))
    cross.append(near.pop())
    for quarter in near + cross:
        source, _ = lax.optimization_barrier((quarter, gated))
        far.append(side_swap(source, 1))
    parts = [*near, *cross, *far]
    experts = [w_gate[0], w_up[0], w_down[0]]

    def slot(shared, lead, dtype):
        solid = ([out_proj] if len(lead) == 3 else []) + experts
        weights = solid + parts
        return call(
            slot_kernel,
            [((rows, width), dtype)],
            place,
            shared,
            *lead,
            *weights,
            specs=[SCALAR] + [VECTOR] * (1 + len(lead)) + [REMOTE] * len(weights),
            scratch=[pltpu.VMEM(array.shape, array.dtype) for array in solid + experts]
            + [pltpu.SemaphoreType.DMA((len(weights),))],
            vmem=VMEM_SLOT,
            flops=2 * rows * part_size(weights),
            expert_count=places,
            given=len(lead),
            count=len(weights),
        )[0]

    routed_late, _ = lax.optimization_barrier((routed, stat))
    shares = [routed]
    for back in range(1, RING):
        shares.append(ring_shift(routed_late, back))
    gain = ffn_gain[None, :]
    lead_one = ring_shift(resid)
    lead_two = ring_shift(lax.optimization_barrier((lead_one, *fars))[0])
    gated_one = ring_shift(gated)
    gated_two = ring_shift(gated_one)
    mix, norm = call(
        own_mix_kernel,
        [((rows, width), jnp.float32), ((rows, width), jnp.bfloat16)],
        gated,
        resid,
        gain,
        out_proj,
        flops=2 * rows * out_proj.size,
    )
    norm_next = ring_shift(norm, -1)
    b16, f32 = jnp.bfloat16, jnp.float32
    part_two = slot(shares[2], (gated_two, lead_two, gain), b16)
    sum_two = ring_shift(part_two)
    part_one = slot(shares[1], (gated_one, lead_one, gain), b16)
    sum_one = ring_shift(part_one, -1)
    part_next = slot(shares[3], (norm_next,), b16)
    sum_next = ring_shift((part_next.astype(f32) + sum_two.astype(f32)).astype(b16))
    total = slot(routed, (norm, mix), f32)
    total = total + sum_one.astype(f32) + sum_next.astype(f32)
    return total.astype(jnp.bfloat16)


def slot_select(expert_ids, expert_count, capacity):
    flat_ids = expert_ids.reshape(-1)
    one_hot = (flat_ids[:, None] == jnp.arange(expert_count, dtype=jnp.int32)[None, :]).astype(
        jnp.int32
    )
    slot_rank = jnp.sum((jnp.cumsum(one_hot, axis=0) - 1) * one_hot, axis=1)
    target = flat_ids * capacity + slot_rank
    return (
        jnp.arange(expert_count * capacity, dtype=jnp.int32)[:, None] == target[None, :]
    ).astype(jnp.bfloat16)


def run_experts(arrived, w_gate, w_up, w_down, sources):
    local_count = w_gate.shape[0]
    grouped = arrived.reshape(sources, local_count, arrived.shape[1], arrived.shape[2])
    gate_pre = jnp.einsum("pesd,edf->pesf", grouped, w_gate, preferred_element_type=jnp.float32)
    up_pre = jnp.einsum("pesd,edf->pesf", grouped, w_up, preferred_element_type=jnp.float32)
    active = (jax.nn.silu(gate_pre) * up_pre).astype(jnp.bfloat16)
    result = jnp.einsum(
        "pesf,efd->pesd", active, w_down, preferred_element_type=jnp.float32
    ).astype(jnp.bfloat16)
    return result.reshape(arrived.shape)


def shards(
    resid,
    query,
    keys,
    values,
    out_gate,
    forget_pre,
    input_pre,
    head_gain,
    out_proj,
    ffn_gain,
    routes,
    route_scores,
    w_gate,
    w_up,
    w_down,
):
    local_heads = forget_pre.shape[0]
    seq_len = query.shape[0]
    head_width = query.shape[1] // local_heads
    heads = [
        cell_head(
            query[:, head * head_width : (head + 1) * head_width],
            keys[:, head * head_width : (head + 1) * head_width],
            values[:, head * head_width : (head + 1) * head_width],
            forget_pre[head : head + 1],
            input_pre[head : head + 1],
        )
        for head in range(local_heads)
    ]
    cell_parts = heads[0][1]
    cell_rows = jnp.concatenate([head[0] for head in heads], axis=1)
    if ring_fits() and w_gate.shape[0] == 1 and local_heads == 1 and w_gate.shape[2] % 512 == 0:
        tokens = seq_len // lax.axis_size("tp")
        token_heads = lax.all_to_all(
            cell_rows.reshape(-1, tokens, head_width), "tp", split_axis=0, concat_axis=0, tiled=True
        )
        gated = call(
            gate_kernel,
            [((tokens, out_gate.shape[1]), jnp.bfloat16)],
            token_heads,
            out_gate,
            head_gain[None, :],
        )[0]
        lead_in = (resid, routes, route_scores)
        return ring_experts(lead_in, cell_parts, gated, ffn_gain, out_proj, w_gate, w_up, w_down)
    token_rows = lax.all_to_all(cell_rows, "tp", split_axis=0, concat_axis=1, tiled=True)
    wide = resid.shape
    after_mix, normed_rows = call(
        mix_kernel,
        [(wide, jnp.float32), (wide, jnp.bfloat16)],
        token_rows,
        out_gate,
        head_gain[None, :],
        out_proj,
        resid,
        ffn_gain[None, :],
    )
    row_count = normed_rows.shape[0]
    half_rows = row_count // 2
    route_count = routes.shape[1]
    sources = lax.axis_size("sp")
    expert_count = w_gate.shape[0] * sources
    capacity = max(2, 2 * half_rows * route_count // expert_count)
    selects = [
        slot_select(
            routes[half_idx * half_rows : (half_idx + 1) * half_rows], expert_count, capacity
        )
        for half_idx in range(2)
    ]

    def pack_rows(half_idx):
        selection = (
            selects[half_idx].reshape(expert_count * capacity, half_rows, route_count).sum(axis=2)
        )
        packed = jnp.dot(
            selection,
            normed_rows[half_idx * half_rows : (half_idx + 1) * half_rows],
            preferred_element_type=jnp.float32,
        )
        return packed.astype(jnp.bfloat16).reshape(expert_count, capacity, normed_rows.shape[1])

    send_rows = jnp.concatenate([pack_rows(0), pack_rows(1)], axis=1)
    finished = run_experts(
        lax.all_to_all(send_rows, "sp", split_axis=0, concat_axis=0, tiled=True),
        w_gate,
        w_up,
        w_down,
        sources,
    )
    returned = lax.all_to_all(finished, "sp", split_axis=0, concat_axis=0, tiled=True)
    answers = [returned[:, :capacity], returned[:, capacity:]]
    route_weight = route_scores / jnp.sum(route_scores, axis=1, keepdims=True)
    pieces = []
    for half_idx in range(2):
        gathered = lax.dot_general(
            selects[half_idx],
            answers[half_idx].reshape(expert_count * capacity, -1),
            (((0,), (0,)), ((), ())),
            preferred_element_type=jnp.float32,
        )
        weights_half = route_weight[half_idx * half_rows : (half_idx + 1) * half_rows]
        pieces.append(
            jnp.sum(gathered.reshape(half_rows, route_count, -1) * weights_half[:, :, None], axis=1)
        )
    return (after_mix + jnp.concatenate(pieces, axis=0)).astype(jnp.bfloat16)


def solution(mesh):
    placed = (
        P(("sp", "tp"), None),
        P("sp", "tp"),
        P("sp", "tp"),
        P("sp", "tp"),
        P(("sp", "tp"), None),
        P("tp", "sp"),
        P("tp", "sp"),
        P(),
        P(),
        P(),
        P(("sp", "tp"), None),
        P(("sp", "tp"), None),
        P("sp", None, None),
        P("sp", None, None),
        P("sp", None, None),
    )
    return jax.shard_map(
        shards, mesh=mesh, in_specs=placed, out_specs=P(("sp", "tp"), None), check_vma=False
    )
```

```python
import functools
import math

import jax
import jax.numpy as jnp
from jax import lax
from jax.experimental import pallas as pl
from jax.experimental.pallas import tpu as pltpu
from jax.sharding import PartitionSpec as P


BLOCK = 64
EPS = 1e-06
FLOOR_LOG = -1e30
AUX_ROWS = 8


def dot(a, b, contract):
    return lax.dot_general(a, b, (contract, ((), ())), preferred_element_type=jnp.float32)


def iota(shape, axis):
    return lax.broadcasted_iota(jnp.int32, shape, axis)


def split_three(x):
    first = x.astype(jnp.bfloat16)
    rest = x - first.astype(jnp.float32)
    second = rest.astype(jnp.bfloat16)
    third = (rest - second.astype(jnp.float32)).astype(jnp.bfloat16)
    return first, second, third


def split_two(x):
    first = x.astype(jnp.bfloat16)
    return first, (x - first.astype(jnp.float32)).astype(jnp.bfloat16)


def pick_rows(rows, count, width):
    row = iota((count, width), 0)
    out = jnp.zeros((count, width), jnp.float32)
    for index, value in enumerate(rows):
        out = jnp.where(row == index, value, out)
    return out


def to_column(row, size):
    eye = iota((size, size), 0) == iota((size, size), 1)
    return jnp.sum(jnp.where(eye, row, 0.0), axis=1, keepdims=True)


def pack_aux(vec, top, total, width):
    return pick_rows([vec, top, total, jnp.ones((1, 1), jnp.float32)], AUX_ROWS, width)


def unpack_aux(aux):
    valid = aux[3:4] > 0.5
    return aux[0:1], jnp.where(valid, aux[1:2], FLOOR_LOG)[:, :1], aux[2:3, :1]


def state_kernel(k_ref, v_ref, forget_ref, input_ref, send_ref, mat_ref, aux_ref, gates_ref, *, chunk):
    seq_len, width = k_ref.shape
    pre = jnp.broadcast_to(forget_ref[...], (8, seq_len))
    log_forget = jnp.minimum(pre, 0.0) - jnp.log1p(jnp.exp(-jnp.abs(pre)))
    cum = jnp.zeros((8, seq_len), jnp.float32)
    upper = (iota((seq_len, seq_len), 0) <= iota((seq_len, seq_len), 1)).astype(jnp.bfloat16)
    for part in reversed(split_three(log_forget)):
        cum = cum + dot(part, upper, ((1,), (0,)))
    level = input_ref[...] - cum
    gates_ref[...] = jnp.where(iota((8, seq_len), 0) == 0, level, cum)
    top = jnp.max(level[:1], axis=1, keepdims=True)
    total = jnp.sum(jnp.where(iota((1, seq_len), 1) == seq_len - 1, cum[:1], 0.0), axis=1, keepdims=True)
    weight = jnp.exp(level[:1] - top)
    mat = jnp.zeros((width, width), jnp.float32)
    vec = jnp.zeros((1, width), jnp.float32)
    for start in range(0, seq_len, chunk):
        here = slice(start, start + chunk)
        column = to_column(weight[:, here], chunk) * width ** (-0.5)
        scaled = k_ref[here, :].astype(jnp.float32) * column
        for part in split_two(scaled):
            vec = vec + jnp.sum(part.astype(jnp.float32), axis=0, keepdims=True)
            mat = mat + dot(part, v_ref[here, :], ((0,), (0,)))
    last = top + total
    mat_ref[...] = mat
    aux_ref[...] = pick_rows([vec, last, total], 8, width)
    send_ref[:width, :] = mat
    send_ref[width:, :] = pack_aux(vec, last, total, width)


def local_kernel(q_ref, k_ref, v_ref, gates_ref, num_ref, stat_ref, *, chunk):
    seq_len, width = q_ref.shape
    key_scale = width ** (-0.5)
    for start in range(0, seq_len, chunk):
        end = start + chunk
        here = slice(start, end)
        scores = dot(q_ref[here, :], k_ref[:end, :], ((1,), (1,))) * key_scale
        row = iota((chunk, end), 0) + start
        col = iota((chunk, end), 1)
        level = jnp.where(col <= row, gates_ref[0:1, :end], -jnp.inf)
        top = jnp.max(level, axis=1, keepdims=True)
        weight = scores * jnp.exp(level - top)
        first = weight.astype(jnp.bfloat16)
        rest = weight - first.astype(jnp.float32)
        own_block = col >= (row // BLOCK) * BLOCK
        second = jnp.where(own_block, 0.0, rest).astype(jnp.bfloat16)
        num_ref[here, :] = dot(first, v_ref[:end, :], ((1,), (0,))) + dot(
            second, v_ref[:end, :], ((1,), (0,))
        )
        den = jnp.sum(first.astype(jnp.float32) + second.astype(jnp.float32), axis=1, keepdims=True)
        cum = to_column(gates_ref[1:2, here], chunk)
        lane = iota((chunk, 128), 1)
        stat_ref[here, :] = jnp.where(lane == 0, den, jnp.where(lane == 1, top, cum))


def merge(old, new):
    old_mat, old_vec, old_max, old_total = old
    new_mat, new_vec, new_max, new_total = new
    joined = jnp.maximum(new_total + old_max, new_max)
    keep_old = jnp.exp(new_total + old_max - joined)
    keep_new = jnp.exp(new_max - joined)
    return (
        keep_old * old_mat + keep_new * new_mat,
        keep_old * old_vec + keep_new * new_vec,
        joined,
        old_total + new_total,
    )


def read_state(mat_ref, aux_ref):
    return (mat_ref[...], aux_ref[0:1, :], aux_ref[1:2, :1], aux_ref[2:3, :1])


def write_state(state, mat_ref, aux_ref):
    mat_ref[...] = state[0]
    aux_ref[...] = pick_rows(state[1:], 8, state[0].shape[1])


def join_kernel(got_ref, mat_ref, aux_ref, far_mat_ref, far_aux_ref, send_ref, mat_out, aux_out, far_mat_out, far_aux_out):
    width = mat_ref.shape[0]
    got = (got_ref[:width, :],) + unpack_aux(got_ref[width:, :])
    state = merge(got, read_state(mat_ref, aux_ref))
    write_state(state, mat_out, aux_out)
    write_state(merge(got, read_state(far_mat_ref, far_aux_ref)), far_mat_out, far_aux_out)
    send_ref[:width, :] = state[0]
    send_ref[width:, :] = pack_aux(*state[1:], width)


def masked(state, valid):
    mat, vec, top, total = state
    return (
        jnp.where(valid, mat, 0.0),
        jnp.where(valid, vec, 0.0),
        jnp.where(valid, top, FLOOR_LOG),
        jnp.where(valid, total, 0.0),
    )


def read_sent(ref):
    rows = ref.shape[0] - AUX_ROWS
    return (ref[:rows, :],) + unpack_aux(ref[rows:, :])


def pair_kernel(place_ref, got_ref, mat_ref, aux_ref, send_ref):
    width = mat_ref.shape[0]
    odd = place_ref[0] % 2 == 1
    own, other = read_state(mat_ref, aux_ref), read_sent(got_ref)
    early = [jnp.where(odd, b, a) for a, b in zip(own, other)]
    late = [jnp.where(odd, a, b) for a, b in zip(own, other)]
    mat, *rest = merge(early, late)
    half = width // 2
    send_ref[:half, :] = jnp.where(odd, mat[half:], mat[:half])
    send_ref[half:, :] = pack_aux(*rest, width)


def read_out(far, q_ref, num_ref, stat_ref, out_ref, chunk):
    mat, vec, far_max, _ = far
    mats = split_three(mat)
    for start in range(0, q_ref.shape[0], chunk):
        here = slice(start, start + chunk)
        query = q_ref[here, :]
        den, top, cum = (stat_ref[here, index : index + 1] for index in range(3))
        joined = jnp.maximum(top, far_max)
        keep_own = jnp.exp(top - joined)
        keep_far = jnp.exp(far_max - joined)
        far_num = sum(dot(query, part, ((1,), (0,))) for part in reversed(mats))
        far_den = jnp.sum(query.astype(jnp.float32) * vec, axis=1, keepdims=True)
        num = keep_own * num_ref[here, :] + keep_far * far_num
        den = keep_own * den + keep_far * far_den
        floor = jnp.exp(-(cum + joined))
        out_ref[here, :] = (num / jnp.maximum(jnp.abs(den), floor)).astype(jnp.bfloat16)


def finish_kernel(got_ref, far_mat_ref, far_aux_ref, q_ref, num_ref, stat_ref, out_ref, *, chunk):
    far = merge(read_sent(got_ref), read_state(far_mat_ref, far_aux_ref))
    read_out(far, q_ref, num_ref, stat_ref, out_ref, chunk)


def far_kernel(place_ref, *refs):
    gots, (mat_ref, aux_ref) = refs[:-2], refs[-2:]
    outer = place_ref[0] // 2
    far = (jnp.zeros(mat_ref.shape, jnp.float32), jnp.zeros((1, mat_ref.shape[1]), jnp.float32))
    far += (jnp.full((1, 1), FLOOR_LOG, jnp.float32), jnp.zeros((1, 1), jnp.float32))
    for back in range(len(gots), 0, -1):
        far = merge(far, masked(read_sent(gots[back - 1]), outer >= back))
    write_state(far, mat_ref, aux_ref)


def finish_pairs_kernel(place_ref, pair_ref, own_ref, other_ref, aux_ref, q_ref, num_ref, stat_ref, out_ref, *, chunk):
    odd = place_ref[0] % 2 == 1
    own, other = own_ref[...], other_ref[...]
    mat = jnp.concatenate([jnp.where(odd, other, own), jnp.where(odd, own, other)], axis=0)
    far = (mat, aux_ref[0:1, :], aux_ref[1:2, :1], aux_ref[2:3, :1])
    far = merge(far, masked(read_sent(pair_ref), odd))
    read_out(far, q_ref, num_ref, stat_ref, out_ref, chunk)


def call(kernel, outs, *args, specs=None, scratch=(), vmem=16, flops=0, **kwargs):
    extra = {} if specs is None else {"in_specs": specs}
    if flops:
        extra["cost_estimate"] = pl.CostEstimate(flops=flops, transcendentals=0, bytes_accessed=0)
    return pl.pallas_call(
        functools.partial(kernel, **kwargs),
        out_shape=[jax.ShapeDtypeStruct(shape, dtype) for shape, dtype in outs],
        scratch_shapes=scratch,
        compiler_params=pltpu.CompilerParams(vmem_limit_bytes=vmem * 2**20),
        **extra,
    )(*args)


SCALAR = pl.BlockSpec(memory_space=pltpu.SMEM)
VECTOR = pl.BlockSpec(memory_space=pltpu.VMEM)
REMOTE = pl.BlockSpec(memory_space=pltpu.HBM)
RING = 4
VMEM_SLOT = 36


def ring_shift(array, step=1):
    places = lax.axis_size("sp")
    return lax.ppermute(array, "sp", [(place, (place + 2 * step) % places) for place in range(places)])


def pair_swap(array):
    return lax.ppermute(array, "sp", [(place, place ^ 1) for place in range(lax.axis_size("sp"))])


def side_swap(array, distance):
    return lax.ppermute(array, "tp", [(place, place ^ distance) for place in range(lax.axis_size("tp"))])


def ring_fits():
    places = lax.axis_size("sp")
    return places == 2 * RING and lax.axis_size("tp") % 4 == 0


def cell_head(query, keys, values, forget_pre, input_pre):
    seq_len, width = query.shape
    chunk = math.gcd(seq_len, 128)
    f32, b16 = jnp.float32, jnp.bfloat16
    states = [((width, width), f32), ((8, width), f32)]
    sent = [((width + AUX_ROWS, width), f32)]
    send, mat, aux, gates = call(
        state_kernel,
        sent + states + [((8, seq_len), f32)],
        keys,
        values,
        forget_pre,
        input_pre,
        vmem=56,
        chunk=chunk,
    )
    num, stat = call(
        local_kernel, [((seq_len, width), f32), ((seq_len, 128), f32)], query, keys, values, gates, chunk=chunk
    )
    if ring_fits():
        place = lax.axis_index("sp").astype(jnp.int32).reshape(1)
        pair = pair_swap(send)
        half = [((width // 2 + AUX_ROWS, width), f32)]
        slab = call(pair_kernel, half, place, pair, mat, aux, specs=[SCALAR] + [VECTOR] * 3)[0]
        far_count = lax.axis_size("sp") // 2 - 1
        fars = []
        for back in range(far_count):
            fars.append(ring_shift(slab, back + 1))
        far_half, far_aux = call(
            far_kernel,
            [((width // 2, width), f32), ((8, width), f32)],
            place,
            *fars,
            specs=[SCALAR] + [VECTOR] * far_count,
        )
        other_half = pair_swap(far_half)
        operands = [pair, far_half, other_half, far_aux, query, num, stat]
        rows = call(
            finish_pairs_kernel,
            [((seq_len, width), b16)],
            place,
            *operands,
            specs=[SCALAR] + [VECTOR] * len(operands),
            chunk=chunk,
        )[0]
        return rows, (send, stat, fars, far_half, rows)
    far_mat = jnp.zeros((width, width), f32)
    far_aux = jnp.where(iota((8, width), 0) == 1, FLOOR_LOG, 0.0)
    places = lax.axis_size("sp")
    step = 1
    got = jnp.zeros(sent[0][0], f32)
    while step < places:
        got = lax.ppermute(send, "sp", [(place, place + step) for place in range(places - step)])
        step *= 2
        if step < places:
            send, mat, aux, far_mat, far_aux = call(
                join_kernel, sent + states + states, got, mat, aux, far_mat, far_aux
            )
    rows = call(
        finish_kernel, [((seq_len, width), b16)], got, far_mat, far_aux, query, num, stat, chunk=chunk
    )[0]
    return rows, got


def mix_kernel(rows_ref, gate_ref, gain_ref, proj_ref, resid_ref, ffn_gain_ref, mix_ref, norm_ref):
    rows = rows_ref[...].astype(jnp.float32)
    headed = rows * lax.rsqrt(jnp.mean(rows * rows, axis=1, keepdims=True) + EPS) * gain_ref[...]
    gated = (headed * jax.nn.sigmoid(gate_ref[...].astype(jnp.float32))).astype(jnp.bfloat16)
    mix = resid_ref[...].astype(jnp.float32) + dot(gated, proj_ref[...], ((1,), (0,)))
    mix_ref[...] = mix
    norm = mix * lax.rsqrt(jnp.mean(mix * mix, axis=1, keepdims=True) + EPS) * ffn_gain_ref[...]
    norm_ref[...] = norm.astype(jnp.bfloat16)


def gate_kernel(heads_ref, gate_ref, gain_ref, out_ref):
    count, _, width = heads_ref.shape
    heads = [heads_ref[head].astype(jnp.float32) for head in range(count)]
    squares = sum(jnp.sum(rows * rows, axis=1, keepdims=True) for rows in heads)
    scale = lax.rsqrt(squares / (count * width) + EPS)
    for head, rows in enumerate(heads):
        here = slice(head * width, (head + 1) * width)
        gate = jax.nn.sigmoid(gate_ref[:, here].astype(jnp.float32))
        out_ref[:, here] = (rows * scale * gain_ref[:, here] * gate).astype(jnp.bfloat16)


def route_kernel(routes_ref, scores_ref, out_ref, *, expert_count):
    scores = scores_ref[...]
    weight = scores / jnp.sum(scores, axis=0, keepdims=True)
    row = iota(out_ref.shape, 0)
    dense = jnp.zeros(out_ref.shape, jnp.float32)
    for route in range(scores.shape[0]):
        named = row % expert_count == routes_ref[route : route + 1, :]
        dense = dense + jnp.where(named, weight[route : route + 1, :], 0.0)
    first, second, third = (part.astype(jnp.float32) for part in split_three(dense))
    place = row // expert_count
    packed = jnp.where(place == 0, first, jnp.where(place == 1, second, third))
    out_ref[...] = jnp.where(place < 3, packed, 0.0).astype(jnp.bfloat16)


def expert_weight(route_ref, expert_count, expert):
    row = iota(route_ref.shape, 0)
    mine = (row % expert_count == expert) & (row < 3 * expert_count)
    weight = jnp.sum(jnp.where(mine, route_ref[...].astype(jnp.float32), 0.0), axis=0, keepdims=True)
    return to_column(weight, route_ref.shape[1])


def mix_rows(gated_ref, resid_ref, proj, gain_ref):
    mix = resid_ref[...].astype(jnp.float32) + dot(gated_ref[...], proj, ((1,), (0,)))
    norm = mix * lax.rsqrt(jnp.mean(mix * mix, axis=1, keepdims=True) + EPS) * gain_ref[...]
    return mix, norm.astype(jnp.bfloat16)


def own_mix_kernel(gated_ref, resid_ref, gain_ref, proj_ref, mix_ref, norm_ref):
    mix_ref[...], norm_ref[...] = mix_rows(gated_ref, resid_ref, proj_ref[...], gain_ref)


def slot_kernel(place_ref, route_ref, *refs, expert_count, given, count):
    lead, sources, out_ref = refs[:given], refs[given : given + count], refs[given + count]
    places, sems = refs[given + count + 1 : -1], refs[-1]
    solid = count - 12
    targets = list(places[:solid])
    _, part = sources[solid].shape
    for index in range(4):
        here = pl.ds(index * part, part)
        targets += [
            places[solid].at[:, here],
            places[solid + 1].at[:, here],
            places[solid + 2].at[here, :],
        ]
    copies = [
        pltpu.make_async_copy(source, target, sems.at[index])
        for index, (source, target) in enumerate(zip(sources, targets))
    ]
    order = list(range(solid))
    order += [solid + 3 * quarter + kind for kind in range(3) for quarter in range(4)]
    for index in order:
        copies[index].start()

    def ready(place):
        for index in [place] if place < solid else range(place, count, 3):
            copies[index].wait()
        return places[place][...]

    if solid == 4:
        gated_ref, resid_ref, gain_ref = lead
        _, rows = mix_rows(gated_ref, resid_ref, ready(0), gain_ref)
    else:
        rows = lead[0][...]

    def expert_part(first):
        gate = dot(rows, ready(first), ((1,), (0,)))
        up = dot(rows, ready(first + 1), ((1,), (0,)))
        active = (jax.nn.silu(gate) * up).astype(jnp.bfloat16)
        return dot(active, ready(first + 2), ((1,), (0,))).astype(jnp.bfloat16).astype(jnp.float32)

    place = place_ref[0]
    other = place + 1 - 2 * (place % 2)
    total = expert_part(solid - 3) * expert_weight(route_ref, expert_count, place)
    total = total + expert_part(solid) * expert_weight(route_ref, expert_count, other)
    if given == 2:
        total = total + lead[1][...]
    out_ref[...] = total.astype(out_ref.dtype)


def part_size(arrays):
    return sum(math.prod(array.shape) for array in arrays)


def ring_experts(lead_in, cell_parts, gated, ffn_gain, out_proj, w_gate, w_up, w_down):
    resid, routes, route_scores = lead_in
    places = lax.axis_size("sp")
    rows, width = resid.shape
    place = lax.axis_index("sp").astype(jnp.int32).reshape(1)
    names = -(-3 * places // 16) * 16
    routed = call(
        route_kernel, [((names, rows), jnp.bfloat16)], routes.T, route_scores.T, expert_count=places
    )[0]
    send, stat, fars, far_half, cell_rows = cell_parts
    part = w_gate.shape[2] // 4
    quarter = lax.axis_index("tp") % 4
    quarters = [
        lax.dynamic_slice_in_dim(w_gate[0], quarter * part, part, 1),
        lax.dynamic_slice_in_dim(w_up[0], quarter * part, part, 1),
        lax.dynamic_slice_in_dim(w_down[0], quarter * part, part, 0),
        lax.dynamic_slice_in_dim(w_down[0], (quarter ^ 2) * part, part, 0),
    ]
    quarters, _ = lax.optimization_barrier((quarters, send))
    near, cross, far = [], [], []
    quarters[2:], _ = lax.optimization_barrier((quarters[2:], far_half))
    for index in range(4):
        near.append(pair_swap(quarters[index]))
    for index, token in enumerate((stat, cell_rows)):
        source, _ = lax.optimization_barrier((near[index], token))
        cross.append(side_swap(source, 2))
    cross.append(near.pop())
    for quarter in near + cross:
        source, _ = lax.optimization_barrier((quarter, gated))
        far.append(side_swap(source, 1))
    parts = [*near, *cross, *far]
    experts = [w_gate[0], w_up[0], w_down[0]]

    def slot(shared, lead, dtype):
        solid = ([out_proj] if len(lead) == 3 else []) + experts
        weights = solid + parts
        return call(
            slot_kernel,
            [((rows, width), dtype)],
            place,
            shared,
            *lead,
            *weights,
            specs=[SCALAR] + [VECTOR] * (1 + len(lead)) + [REMOTE] * len(weights),
            scratch=[pltpu.VMEM(array.shape, array.dtype) for array in solid + experts]
            + [pltpu.SemaphoreType.DMA((len(weights),))],
            vmem=VMEM_SLOT,
            flops=2 * rows * part_size(weights),
            expert_count=places,
            given=len(lead),
            count=len(weights),
        )[0]

    routed_late, _ = lax.optimization_barrier((routed, send))
    shares = [routed]
    for back in range(1, RING):
        shares.append(ring_shift(routed_late, back))
    gain = ffn_gain[None, :]
    lead_one = ring_shift(resid)
    lead_two = ring_shift(lax.optimization_barrier((lead_one, *fars))[0])
    gated_one = ring_shift(gated)
    gated_two = ring_shift(gated_one)
    mix, norm = call(
        own_mix_kernel,
        [((rows, width), jnp.float32), ((rows, width), jnp.bfloat16)],
        gated,
        resid,
        gain,
        out_proj,
        flops=2 * rows * out_proj.size,
    )
    norm_next = ring_shift(norm, -1)
    b16, f32 = jnp.bfloat16, jnp.float32
    part_two = slot(shares[2], (gated_two, lead_two, gain), b16)
    sum_two = ring_shift(part_two)
    part_one = slot(shares[1], (gated_one, lead_one, gain), b16)
    sum_one = ring_shift(part_one, -1)
    part_next = slot(shares[3], (norm_next,), b16)
    sum_next = ring_shift((part_next.astype(f32) + sum_two.astype(f32)).astype(b16))
    total = slot(routed, (norm, mix), f32)
    total = total + sum_one.astype(f32) + sum_next.astype(f32)
    return total.astype(jnp.bfloat16)


def slot_select(expert_ids, expert_count, capacity):
    flat_ids = expert_ids.reshape(-1)
    one_hot = (flat_ids[:, None] == jnp.arange(expert_count, dtype=jnp.int32)[None, :]).astype(
        jnp.int32
    )
    slot_rank = jnp.sum((jnp.cumsum(one_hot, axis=0) - 1) * one_hot, axis=1)
    target = flat_ids * capacity + slot_rank
    return (
        jnp.arange(expert_count * capacity, dtype=jnp.int32)[:, None] == target[None, :]
    ).astype(jnp.bfloat16)


def run_experts(arrived, w_gate, w_up, w_down, sources):
    local_count = w_gate.shape[0]
    grouped = arrived.reshape(sources, local_count, arrived.shape[1], arrived.shape[2])
    gate_pre = jnp.einsum("pesd,edf->pesf", grouped, w_gate, preferred_element_type=jnp.float32)
    up_pre = jnp.einsum("pesd,edf->pesf", grouped, w_up, preferred_element_type=jnp.float32)
    active = (jax.nn.silu(gate_pre) * up_pre).astype(jnp.bfloat16)
    result = jnp.einsum(
        "pesf,efd->pesd", active, w_down, preferred_element_type=jnp.float32
    ).astype(jnp.bfloat16)
    return result.reshape(arrived.shape)


def shards(
    resid,
    query,
    keys,
    values,
    out_gate,
    forget_pre,
    input_pre,
    head_gain,
    out_proj,
    ffn_gain,
    routes,
    route_scores,
    w_gate,
    w_up,
    w_down,
):
    local_heads = forget_pre.shape[0]
    seq_len = query.shape[0]
    head_width = query.shape[1] // local_heads
    heads = [
        cell_head(
            query[:, head * head_width : (head + 1) * head_width],
            keys[:, head * head_width : (head + 1) * head_width],
            values[:, head * head_width : (head + 1) * head_width],
            forget_pre[head : head + 1],
            input_pre[head : head + 1],
        )
        for head in range(local_heads)
    ]
    cell_parts = heads[0][1]
    cell_rows = jnp.concatenate([head[0] for head in heads], axis=1)
    if ring_fits() and w_gate.shape[0] == 1 and local_heads == 1 and w_gate.shape[2] % 512 == 0:
        tokens = seq_len // lax.axis_size("tp")
        token_heads = lax.all_to_all(
            cell_rows.reshape(-1, tokens, head_width), "tp", split_axis=0, concat_axis=0, tiled=True
        )
        gated = call(
            gate_kernel,
            [((tokens, out_gate.shape[1]), jnp.bfloat16)],
            token_heads,
            out_gate,
            head_gain[None, :],
        )[0]
        lead_in = (resid, routes, route_scores)
        return ring_experts(lead_in, cell_parts, gated, ffn_gain, out_proj, w_gate, w_up, w_down)
    token_rows = lax.all_to_all(cell_rows, "tp", split_axis=0, concat_axis=1, tiled=True)
    wide = resid.shape
    after_mix, normed_rows = call(
        mix_kernel,
        [(wide, jnp.float32), (wide, jnp.bfloat16)],
        token_rows,
        out_gate,
        head_gain[None, :],
        out_proj,
        resid,
        ffn_gain[None, :],
    )
    row_count = normed_rows.shape[0]
    half_rows = row_count // 2
    route_count = routes.shape[1]
    sources = lax.axis_size("sp")
    expert_count = w_gate.shape[0] * sources
    capacity = max(2, 2 * half_rows * route_count // expert_count)
    selects = [
        slot_select(
            routes[half_idx * half_rows : (half_idx + 1) * half_rows], expert_count, capacity
        )
        for half_idx in range(2)
    ]

    def pack_rows(half_idx):
        selection = (
            selects[half_idx].reshape(expert_count * capacity, half_rows, route_count).sum(axis=2)
        )
        packed = jnp.dot(
            selection,
            normed_rows[half_idx * half_rows : (half_idx + 1) * half_rows],
            preferred_element_type=jnp.float32,
        )
        return packed.astype(jnp.bfloat16).reshape(expert_count, capacity, normed_rows.shape[1])

    send_rows = jnp.concatenate([pack_rows(0), pack_rows(1)], axis=1)
    finished = run_experts(
        lax.all_to_all(send_rows, "sp", split_axis=0, concat_axis=0, tiled=True),
        w_gate,
        w_up,
        w_down,
        sources,
    )
    returned = lax.all_to_all(finished, "sp", split_axis=0, concat_axis=0, tiled=True)
    answers = [returned[:, :capacity], returned[:, capacity:]]
    route_weight = route_scores / jnp.sum(route_scores, axis=1, keepdims=True)
    pieces = []
    for half_idx in range(2):
        gathered = lax.dot_general(
            selects[half_idx],
            answers[half_idx].reshape(expert_count * capacity, -1),
            (((0,), (0,)), ((), ())),
            preferred_element_type=jnp.float32,
        )
        weights_half = route_weight[half_idx * half_rows : (half_idx + 1) * half_rows]
        pieces.append(
            jnp.sum(gathered.reshape(half_rows, route_count, -1) * weights_half[:, :, None], axis=1)
        )
    return (after_mix + jnp.concatenate(pieces, axis=0)).astype(jnp.bfloat16)


def solution(mesh):
    placed = (
        P(("sp", "tp"), None),
        P("sp", "tp"),
        P("sp", "tp"),
        P("sp", "tp"),
        P(("sp", "tp"), None),
        P("tp", "sp"),
        P("tp", "sp"),
        P(),
        P(),
        P(),
        P(("sp", "tp"), None),
        P(("sp", "tp"), None),
        P("sp", None, None),
        P("sp", None, None),
        P("sp", None, None),
    )
    return jax.shard_map(
        shards, mesh=mesh, in_specs=placed, out_specs=P(("sp", "tp"), None), check_vma=False
    )
```

```python
import functools
import math

import jax
import jax.numpy as jnp
from jax import lax
from jax.experimental import pallas as pl
from jax.experimental.pallas import tpu as pltpu
from jax.sharding import PartitionSpec as P


BLOCK = 64
EPS = 1e-06
FLOOR_LOG = -1e30
AUX_ROWS = 8


def dot(a, b, contract):
    return lax.dot_general(a, b, (contract, ((), ())), preferred_element_type=jnp.float32)


def iota(shape, axis):
    return lax.broadcasted_iota(jnp.int32, shape, axis)


def split_three(x):
    first = x.astype(jnp.bfloat16)
    rest = x - first.astype(jnp.float32)
    second = rest.astype(jnp.bfloat16)
    third = (rest - second.astype(jnp.float32)).astype(jnp.bfloat16)
    return first, second, third


def split_two(x):
    first = x.astype(jnp.bfloat16)
    return first, (x - first.astype(jnp.float32)).astype(jnp.bfloat16)


def pick_rows(rows, count, width):
    row = iota((count, width), 0)
    out = jnp.zeros((count, width), jnp.float32)
    for index, value in enumerate(rows):
        out = jnp.where(row == index, value, out)
    return out


def to_column(row, size):
    eye = iota((size, size), 0) == iota((size, size), 1)
    return jnp.sum(jnp.where(eye, row, 0.0), axis=1, keepdims=True)


def pack_aux(vec, top, total, width):
    return pick_rows([vec, top, total, jnp.ones((1, 1), jnp.float32)], AUX_ROWS, width)


def unpack_aux(aux):
    valid = aux[3:4] > 0.5
    return aux[0:1], jnp.where(valid, aux[1:2], FLOOR_LOG)[:, :1], aux[2:3, :1]


def state_kernel(k_ref, v_ref, forget_ref, input_ref, send_ref, mat_ref, aux_ref, gates_ref, *, chunk):
    seq_len, width = k_ref.shape
    pre = jnp.broadcast_to(forget_ref[...], (8, seq_len))
    log_forget = jnp.minimum(pre, 0.0) - jnp.log1p(jnp.exp(-jnp.abs(pre)))
    cum = jnp.zeros((8, seq_len), jnp.float32)
    upper = (iota((seq_len, seq_len), 0) <= iota((seq_len, seq_len), 1)).astype(jnp.bfloat16)
    for part in reversed(split_three(log_forget)):
        cum = cum + dot(part, upper, ((1,), (0,)))
    level = input_ref[...] - cum
    gates_ref[...] = jnp.where(iota((8, seq_len), 0) == 0, level, cum)
    top = jnp.max(level[:1], axis=1, keepdims=True)
    total = jnp.sum(jnp.where(iota((1, seq_len), 1) == seq_len - 1, cum[:1], 0.0), axis=1, keepdims=True)
    weight = jnp.exp(level[:1] - top)
    mat = jnp.zeros((width, width), jnp.float32)
    vec = jnp.zeros((1, width), jnp.float32)
    for start in range(0, seq_len, chunk):
        here = slice(start, start + chunk)
        column = to_column(weight[:, here], chunk) * width ** (-0.5)
        scaled = k_ref[here, :].astype(jnp.float32) * column
        for part in split_two(scaled):
            vec = vec + jnp.sum(part.astype(jnp.float32), axis=0, keepdims=True)
            mat = mat + dot(part, v_ref[here, :], ((0,), (0,)))
    last = top + total
    mat_ref[...] = mat
    aux_ref[...] = pick_rows([vec, last, total], 8, width)
    send_ref[:width, :] = mat
    send_ref[width:, :] = pack_aux(vec, last, total, width)


def local_kernel(q_ref, k_ref, v_ref, gates_ref, num_ref, stat_ref, *, chunk):
    seq_len, width = q_ref.shape
    key_scale = width ** (-0.5)
    for start in range(0, seq_len, chunk):
        end = start + chunk
        here = slice(start, end)
        scores = dot(q_ref[here, :], k_ref[:end, :], ((1,), (1,))) * key_scale
        row = iota((chunk, end), 0) + start
        col = iota((chunk, end), 1)
        level = jnp.where(col <= row, gates_ref[0:1, :end], -jnp.inf)
        top = jnp.max(level, axis=1, keepdims=True)
        weight = scores * jnp.exp(level - top)
        first = weight.astype(jnp.bfloat16)
        rest = weight - first.astype(jnp.float32)
        own_block = col >= (row // BLOCK) * BLOCK
        second = jnp.where(own_block, 0.0, rest).astype(jnp.bfloat16)
        num_ref[here, :] = dot(first, v_ref[:end, :], ((1,), (0,))) + dot(
            second, v_ref[:end, :], ((1,), (0,))
        )
        den = jnp.sum(first.astype(jnp.float32) + second.astype(jnp.float32), axis=1, keepdims=True)
        cum = to_column(gates_ref[1:2, here], chunk)
        lane = iota((chunk, 128), 1)
        stat_ref[here, :] = jnp.where(lane == 0, den, jnp.where(lane == 1, top, cum))


def merge(old, new):
    old_mat, old_vec, old_max, old_total = old
    new_mat, new_vec, new_max, new_total = new
    joined = jnp.maximum(new_total + old_max, new_max)
    keep_old = jnp.exp(new_total + old_max - joined)
    keep_new = jnp.exp(new_max - joined)
    return (
        keep_old * old_mat + keep_new * new_mat,
        keep_old * old_vec + keep_new * new_vec,
        joined,
        old_total + new_total,
    )


def read_state(mat_ref, aux_ref):
    return (mat_ref[...], aux_ref[0:1, :], aux_ref[1:2, :1], aux_ref[2:3, :1])


def write_state(state, mat_ref, aux_ref):
    mat_ref[...] = state[0]
    aux_ref[...] = pick_rows(state[1:], 8, state[0].shape[1])


def join_kernel(got_ref, mat_ref, aux_ref, far_mat_ref, far_aux_ref, send_ref, mat_out, aux_out, far_mat_out, far_aux_out):
    width = mat_ref.shape[0]
    got = (got_ref[:width, :],) + unpack_aux(got_ref[width:, :])
    state = merge(got, read_state(mat_ref, aux_ref))
    write_state(state, mat_out, aux_out)
    write_state(merge(got, read_state(far_mat_ref, far_aux_ref)), far_mat_out, far_aux_out)
    send_ref[:width, :] = state[0]
    send_ref[width:, :] = pack_aux(*state[1:], width)


def masked(state, valid):
    mat, vec, top, total = state
    return (
        jnp.where(valid, mat, 0.0),
        jnp.where(valid, vec, 0.0),
        jnp.where(valid, top, FLOOR_LOG),
        jnp.where(valid, total, 0.0),
    )


def read_sent(ref):
    rows = ref.shape[0] - AUX_ROWS
    return (ref[:rows, :],) + unpack_aux(ref[rows:, :])


def pair_kernel(place_ref, got_ref, mat_ref, aux_ref, send_ref):
    width = mat_ref.shape[0]
    odd = place_ref[0] % 2 == 1
    own, other = read_state(mat_ref, aux_ref), read_sent(got_ref)
    early = [jnp.where(odd, b, a) for a, b in zip(own, other)]
    late = [jnp.where(odd, a, b) for a, b in zip(own, other)]
    mat, *rest = merge(early, late)
    half = width // 2
    send_ref[:half, :] = jnp.where(odd, mat[half:], mat[:half])
    send_ref[half:, :] = pack_aux(*rest, width)


def read_out(far, q_ref, num_ref, stat_ref, out_ref, chunk):
    mat, vec, far_max, _ = far
    mats = split_three(mat)
    for start in range(0, q_ref.shape[0], chunk):
        here = slice(start, start + chunk)
        query = q_ref[here, :]
        den, top, cum = (stat_ref[here, index : index + 1] for index in range(3))
        joined = jnp.maximum(top, far_max)
        keep_own = jnp.exp(top - joined)
        keep_far = jnp.exp(far_max - joined)
        far_num = sum(dot(query, part, ((1,), (0,))) for part in reversed(mats))
        far_den = jnp.sum(query.astype(jnp.float32) * vec, axis=1, keepdims=True)
        num = keep_own * num_ref[here, :] + keep_far * far_num
        den = keep_own * den + keep_far * far_den
        floor = jnp.exp(-(cum + joined))
        out_ref[here, :] = (num / jnp.maximum(jnp.abs(den), floor)).astype(jnp.bfloat16)


def finish_kernel(got_ref, far_mat_ref, far_aux_ref, q_ref, num_ref, stat_ref, out_ref, *, chunk):
    far = merge(read_sent(got_ref), read_state(far_mat_ref, far_aux_ref))
    read_out(far, q_ref, num_ref, stat_ref, out_ref, chunk)


def far_kernel(place_ref, *refs):
    gots, (mat_ref, aux_ref) = refs[:-2], refs[-2:]
    outer = place_ref[0] // 2
    far = (jnp.zeros(mat_ref.shape, jnp.float32), jnp.zeros((1, mat_ref.shape[1]), jnp.float32))
    far += (jnp.full((1, 1), FLOOR_LOG, jnp.float32), jnp.zeros((1, 1), jnp.float32))
    for back in range(len(gots), 0, -1):
        far = merge(far, masked(read_sent(gots[back - 1]), outer >= back))
    write_state(far, mat_ref, aux_ref)


def finish_pairs_kernel(place_ref, pair_ref, own_ref, other_ref, aux_ref, q_ref, num_ref, stat_ref, out_ref, *, chunk):
    odd = place_ref[0] % 2 == 1
    own, other = own_ref[...], other_ref[...]
    mat = jnp.concatenate([jnp.where(odd, other, own), jnp.where(odd, own, other)], axis=0)
    far = (mat, aux_ref[0:1, :], aux_ref[1:2, :1], aux_ref[2:3, :1])
    far = merge(far, masked(read_sent(pair_ref), odd))
    read_out(far, q_ref, num_ref, stat_ref, out_ref, chunk)


def call(kernel, outs, *args, specs=None, scratch=(), vmem=16, flops=0, **kwargs):
    extra = {} if specs is None else {"in_specs": specs}
    if flops:
        extra["cost_estimate"] = pl.CostEstimate(flops=flops, transcendentals=0, bytes_accessed=0)
    return pl.pallas_call(
        functools.partial(kernel, **kwargs),
        out_shape=[jax.ShapeDtypeStruct(shape, dtype) for shape, dtype in outs],
        scratch_shapes=scratch,
        compiler_params=pltpu.CompilerParams(vmem_limit_bytes=vmem * 2**20),
        **extra,
    )(*args)


SCALAR = pl.BlockSpec(memory_space=pltpu.SMEM)
VECTOR = pl.BlockSpec(memory_space=pltpu.VMEM)
REMOTE = pl.BlockSpec(memory_space=pltpu.HBM)
RING = 4
VMEM_SLOT = 36


def ring_shift(array, step=1):
    places = lax.axis_size("sp")
    return lax.ppermute(array, "sp", [(place, (place + 2 * step) % places) for place in range(places)])


def pair_swap(array):
    return lax.ppermute(array, "sp", [(place, place ^ 1) for place in range(lax.axis_size("sp"))])


def side_swap(array, distance):
    return lax.ppermute(array, "tp", [(place, place ^ distance) for place in range(lax.axis_size("tp"))])


def ring_fits():
    places = lax.axis_size("sp")
    return places == 2 * RING and lax.axis_size("tp") % 4 == 0


def cell_head(query, keys, values, forget_pre, input_pre):
    seq_len, width = query.shape
    chunk = math.gcd(seq_len, 128)
    f32, b16 = jnp.float32, jnp.bfloat16
    states = [((width, width), f32), ((8, width), f32)]
    sent = [((width + AUX_ROWS, width), f32)]
    send, mat, aux, gates = call(
        state_kernel,
        sent + states + [((8, seq_len), f32)],
        keys,
        values,
        forget_pre,
        input_pre,
        vmem=56,
        chunk=chunk,
    )
    num, stat = call(
        local_kernel, [((seq_len, width), f32), ((seq_len, 128), f32)], query, keys, values, gates, chunk=chunk
    )
    if ring_fits():
        place = lax.axis_index("sp").astype(jnp.int32).reshape(1)
        pair = pair_swap(send)
        half = [((width // 2 + AUX_ROWS, width), f32)]
        slab = call(pair_kernel, half, place, pair, mat, aux, specs=[SCALAR] + [VECTOR] * 3)[0]
        far_count = lax.axis_size("sp") // 2 - 1
        fars = []
        for back in range(far_count):
            fars.append(ring_shift(slab, back + 1))
        far_half, far_aux = call(
            far_kernel,
            [((width // 2, width), f32), ((8, width), f32)],
            place,
            *fars,
            specs=[SCALAR] + [VECTOR] * far_count,
        )
        other_half = pair_swap(far_half)
        operands = [pair, far_half, other_half, far_aux, query, num, stat]
        rows = call(
            finish_pairs_kernel,
            [((seq_len, width), b16)],
            place,
            *operands,
            specs=[SCALAR] + [VECTOR] * len(operands),
            chunk=chunk,
        )[0]
        return rows, (send, stat, fars, far_half, rows)
    far_mat = jnp.zeros((width, width), f32)
    far_aux = jnp.where(iota((8, width), 0) == 1, FLOOR_LOG, 0.0)
    places = lax.axis_size("sp")
    step = 1
    got = jnp.zeros(sent[0][0], f32)
    while step < places:
        got = lax.ppermute(send, "sp", [(place, place + step) for place in range(places - step)])
        step *= 2
        if step < places:
            send, mat, aux, far_mat, far_aux = call(
                join_kernel, sent + states + states, got, mat, aux, far_mat, far_aux
            )
    rows = call(
        finish_kernel, [((seq_len, width), b16)], got, far_mat, far_aux, query, num, stat, chunk=chunk
    )[0]
    return rows, got


def mix_kernel(rows_ref, gate_ref, gain_ref, proj_ref, resid_ref, ffn_gain_ref, mix_ref, norm_ref):
    rows = rows_ref[...].astype(jnp.float32)
    headed = rows * lax.rsqrt(jnp.mean(rows * rows, axis=1, keepdims=True) + EPS) * gain_ref[...]
    gated = (headed * jax.nn.sigmoid(gate_ref[...].astype(jnp.float32))).astype(jnp.bfloat16)
    mix = resid_ref[...].astype(jnp.float32) + dot(gated, proj_ref[...], ((1,), (0,)))
    mix_ref[...] = mix
    norm = mix * lax.rsqrt(jnp.mean(mix * mix, axis=1, keepdims=True) + EPS) * ffn_gain_ref[...]
    norm_ref[...] = norm.astype(jnp.bfloat16)


def gate_kernel(heads_ref, gate_ref, gain_ref, out_ref):
    count, _, width = heads_ref.shape
    heads = [heads_ref[head].astype(jnp.float32) for head in range(count)]
    squares = sum(jnp.sum(rows * rows, axis=1, keepdims=True) for rows in heads)
    scale = lax.rsqrt(squares / (count * width) + EPS)
    for head, rows in enumerate(heads):
        here = slice(head * width, (head + 1) * width)
        gate = jax.nn.sigmoid(gate_ref[:, here].astype(jnp.float32))
        out_ref[:, here] = (rows * scale * gain_ref[:, here] * gate).astype(jnp.bfloat16)


def route_kernel(routes_ref, scores_ref, out_ref, *, expert_count):
    scores = scores_ref[...]
    weight = scores / jnp.sum(scores, axis=0, keepdims=True)
    row = iota(out_ref.shape, 0)
    dense = jnp.zeros(out_ref.shape, jnp.float32)
    for route in range(scores.shape[0]):
        named = row % expert_count == routes_ref[route : route + 1, :]
        dense = dense + jnp.where(named, weight[route : route + 1, :], 0.0)
    first, second, third = (part.astype(jnp.float32) for part in split_three(dense))
    place = row // expert_count
    packed = jnp.where(place == 0, first, jnp.where(place == 1, second, third))
    out_ref[...] = jnp.where(place < 3, packed, 0.0).astype(jnp.bfloat16)


def expert_weight(route_ref, expert_count, expert):
    row = iota(route_ref.shape, 0)
    mine = (row % expert_count == expert) & (row < 3 * expert_count)
    weight = jnp.sum(jnp.where(mine, route_ref[...].astype(jnp.float32), 0.0), axis=0, keepdims=True)
    return to_column(weight, route_ref.shape[1])


def mix_rows(gated_ref, resid_ref, proj, gain_ref):
    mix = resid_ref[...].astype(jnp.float32) + dot(gated_ref[...], proj, ((1,), (0,)))
    norm = mix * lax.rsqrt(jnp.mean(mix * mix, axis=1, keepdims=True) + EPS) * gain_ref[...]
    return mix, norm.astype(jnp.bfloat16)


def own_mix_kernel(gated_ref, resid_ref, gain_ref, proj_ref, mix_ref, norm_ref):
    mix_ref[...], norm_ref[...] = mix_rows(gated_ref, resid_ref, proj_ref[...], gain_ref)


def slot_kernel(place_ref, route_ref, *refs, expert_count, given, count):
    lead, sources, out_ref = refs[:given], refs[given : given + count], refs[given + count]
    places, sems = refs[given + count + 1 : -1], refs[-1]
    solid = count - 12
    targets = list(places[:solid])
    _, part = sources[solid].shape
    for index in range(4):
        here = pl.ds(index * part, part)
        targets += [
            places[solid].at[:, here],
            places[solid + 1].at[:, here],
            places[solid + 2].at[here, :],
        ]
    copies = [
        pltpu.make_async_copy(source, target, sems.at[index])
        for index, (source, target) in enumerate(zip(sources, targets))
    ]
    order = list(range(solid))
    order += [solid + 3 * quarter + kind for kind in range(3) for quarter in range(4)]
    for index in order:
        copies[index].start()

    def ready(place):
        for index in [place] if place < solid else range(place, count, 3):
            copies[index].wait()
        return places[place][...]

    if solid == 4:
        gated_ref, resid_ref, gain_ref = lead
        _, rows = mix_rows(gated_ref, resid_ref, ready(0), gain_ref)
    else:
        rows = lead[0][...]

    def expert_part(first):
        gate = dot(rows, ready(first), ((1,), (0,)))
        up = dot(rows, ready(first + 1), ((1,), (0,)))
        active = (jax.nn.silu(gate) * up).astype(jnp.bfloat16)
        return dot(active, ready(first + 2), ((1,), (0,))).astype(jnp.bfloat16).astype(jnp.float32)

    place = place_ref[0]
    other = place + 1 - 2 * (place % 2)
    total = expert_part(solid - 3) * expert_weight(route_ref, expert_count, place)
    total = total + expert_part(solid) * expert_weight(route_ref, expert_count, other)
    if given == 2:
        total = total + lead[1][...]
    out_ref[...] = total.astype(out_ref.dtype)


def part_size(arrays):
    return sum(math.prod(array.shape) for array in arrays)


def ring_experts(lead_in, cell_parts, gated, ffn_gain, out_proj, w_gate, w_up, w_down):
    resid, routes, route_scores = lead_in
    places = lax.axis_size("sp")
    rows, width = resid.shape
    place = lax.axis_index("sp").astype(jnp.int32).reshape(1)
    names = -(-3 * places // 16) * 16
    routed = call(
        route_kernel, [((names, rows), jnp.bfloat16)], routes.T, route_scores.T, expert_count=places
    )[0]
    send, _, fars, far_half, cell_rows = cell_parts
    part = w_gate.shape[2] // 4
    quarter = lax.axis_index("tp") % 4
    quarters = [
        lax.dynamic_slice_in_dim(w_gate[0], quarter * part, part, 1),
        lax.dynamic_slice_in_dim(w_up[0], quarter * part, part, 1),
        lax.dynamic_slice_in_dim(w_down[0], quarter * part, part, 0),
        lax.dynamic_slice_in_dim(w_down[0], (quarter ^ 2) * part, part, 0),
    ]
    quarters, _ = lax.optimization_barrier((quarters, send))
    near, cross, far = [], [], []
    quarters[2:], _ = lax.optimization_barrier((quarters[2:], far_half))
    for index in range(4):
        near.append(pair_swap(quarters[index]))
    for index, token in enumerate((send, cell_rows)):
        source, _ = lax.optimization_barrier((near[index], token))
        cross.append(side_swap(source, 2))
    cross.append(near.pop())
    for quarter in near + cross:
        source, _ = lax.optimization_barrier((quarter, gated))
        far.append(side_swap(source, 1))
    parts = [*near, *cross, *far]
    experts = [w_gate[0], w_up[0], w_down[0]]

    def slot(shared, lead, dtype):
        solid = ([out_proj] if len(lead) == 3 else []) + experts
        weights = solid + parts
        return call(
            slot_kernel,
            [((rows, width), dtype)],
            place,
            shared,
            *lead,
            *weights,
            specs=[SCALAR] + [VECTOR] * (1 + len(lead)) + [REMOTE] * len(weights),
            scratch=[pltpu.VMEM(array.shape, array.dtype) for array in solid + experts]
            + [pltpu.SemaphoreType.DMA((len(weights),))],
            vmem=VMEM_SLOT,
            flops=2 * rows * part_size(weights),
            expert_count=places,
            given=len(lead),
            count=len(weights),
        )[0]

    routed_late, _ = lax.optimization_barrier((routed, cell_rows))
    shares = [routed]
    for back in range(1, RING):
        shares.append(ring_shift(routed_late, back))
    gain = ffn_gain[None, :]
    lead_one = ring_shift(resid)
    lead_two = ring_shift(lax.optimization_barrier((lead_one, *fars))[0])
    gated_one = ring_shift(gated)
    gated_two = ring_shift(gated_one)
    mix, norm = call(
        own_mix_kernel,
        [((rows, width), jnp.float32), ((rows, width), jnp.bfloat16)],
        gated,
        resid,
        gain,
        out_proj,
        flops=2 * rows * out_proj.size,
    )
    norm_next = ring_shift(norm, -1)
    b16, f32 = jnp.bfloat16, jnp.float32
    part_two = slot(shares[2], (gated_two, lead_two, gain), b16)
    sum_two = ring_shift(part_two)
    part_one = slot(shares[1], (gated_one, lead_one, gain), b16)
    sum_one = ring_shift(part_one, -1)
    part_next = slot(shares[3], (norm_next,), b16)
    sum_next = ring_shift((part_next.astype(f32) + sum_two.astype(f32)).astype(b16))
    total = slot(routed, (norm, mix), f32)
    total = total + sum_one.astype(f32) + sum_next.astype(f32)
    return total.astype(jnp.bfloat16)


def slot_select(expert_ids, expert_count, capacity):
    flat_ids = expert_ids.reshape(-1)
    one_hot = (flat_ids[:, None] == jnp.arange(expert_count, dtype=jnp.int32)[None, :]).astype(
        jnp.int32
    )
    slot_rank = jnp.sum((jnp.cumsum(one_hot, axis=0) - 1) * one_hot, axis=1)
    target = flat_ids * capacity + slot_rank
    return (
        jnp.arange(expert_count * capacity, dtype=jnp.int32)[:, None] == target[None, :]
    ).astype(jnp.bfloat16)


def run_experts(arrived, w_gate, w_up, w_down, sources):
    local_count = w_gate.shape[0]
    grouped = arrived.reshape(sources, local_count, arrived.shape[1], arrived.shape[2])
    gate_pre = jnp.einsum("pesd,edf->pesf", grouped, w_gate, preferred_element_type=jnp.float32)
    up_pre = jnp.einsum("pesd,edf->pesf", grouped, w_up, preferred_element_type=jnp.float32)
    active = (jax.nn.silu(gate_pre) * up_pre).astype(jnp.bfloat16)
    result = jnp.einsum(
        "pesf,efd->pesd", active, w_down, preferred_element_type=jnp.float32
    ).astype(jnp.bfloat16)
    return result.reshape(arrived.shape)


def shards(
    resid,
    query,
    keys,
    values,
    out_gate,
    forget_pre,
    input_pre,
    head_gain,
    out_proj,
    ffn_gain,
    routes,
    route_scores,
    w_gate,
    w_up,
    w_down,
):
    local_heads = forget_pre.shape[0]
    seq_len = query.shape[0]
    head_width = query.shape[1] // local_heads
    heads = [
        cell_head(
            query[:, head * head_width : (head + 1) * head_width],
            keys[:, head * head_width : (head + 1) * head_width],
            values[:, head * head_width : (head + 1) * head_width],
            forget_pre[head : head + 1],
            input_pre[head : head + 1],
        )
        for head in range(local_heads)
    ]
    cell_parts = heads[0][1]
    cell_rows = jnp.concatenate([head[0] for head in heads], axis=1)
    if ring_fits() and w_gate.shape[0] == 1 and local_heads == 1 and w_gate.shape[2] % 512 == 0:
        tokens = seq_len // lax.axis_size("tp")
        token_heads = lax.all_to_all(
            cell_rows.reshape(-1, tokens, head_width), "tp", split_axis=0, concat_axis=0, tiled=True
        )
        gated = call(
            gate_kernel,
            [((tokens, out_gate.shape[1]), jnp.bfloat16)],
            token_heads,
            out_gate,
            head_gain[None, :],
        )[0]
        lead_in = (resid, routes, route_scores)
        return ring_experts(lead_in, cell_parts, gated, ffn_gain, out_proj, w_gate, w_up, w_down)
    token_rows = lax.all_to_all(cell_rows, "tp", split_axis=0, concat_axis=1, tiled=True)
    wide = resid.shape
    after_mix, normed_rows = call(
        mix_kernel,
        [(wide, jnp.float32), (wide, jnp.bfloat16)],
        token_rows,
        out_gate,
        head_gain[None, :],
        out_proj,
        resid,
        ffn_gain[None, :],
    )
    row_count = normed_rows.shape[0]
    half_rows = row_count // 2
    route_count = routes.shape[1]
    sources = lax.axis_size("sp")
    expert_count = w_gate.shape[0] * sources
    capacity = max(2, 2 * half_rows * route_count // expert_count)
    selects = [
        slot_select(
            routes[half_idx * half_rows : (half_idx + 1) * half_rows], expert_count, capacity
        )
        for half_idx in range(2)
    ]

    def pack_rows(half_idx):
        selection = (
            selects[half_idx].reshape(expert_count * capacity, half_rows, route_count).sum(axis=2)
        )
        packed = jnp.dot(
            selection,
            normed_rows[half_idx * half_rows : (half_idx + 1) * half_rows],
            preferred_element_type=jnp.float32,
        )
        return packed.astype(jnp.bfloat16).reshape(expert_count, capacity, normed_rows.shape[1])

    send_rows = jnp.concatenate([pack_rows(0), pack_rows(1)], axis=1)
    finished = run_experts(
        lax.all_to_all(send_rows, "sp", split_axis=0, concat_axis=0, tiled=True),
        w_gate,
        w_up,
        w_down,
        sources,
    )
    returned = lax.all_to_all(finished, "sp", split_axis=0, concat_axis=0, tiled=True)
    answers = [returned[:, :capacity], returned[:, capacity:]]
    route_weight = route_scores / jnp.sum(route_scores, axis=1, keepdims=True)
    pieces = []
    for half_idx in range(2):
        gathered = lax.dot_general(
            selects[half_idx],
            answers[half_idx].reshape(expert_count * capacity, -1),
            (((0,), (0,)), ((), ())),
            preferred_element_type=jnp.float32,
        )
        weights_half = route_weight[half_idx * half_rows : (half_idx + 1) * half_rows]
        pieces.append(
            jnp.sum(gathered.reshape(half_rows, route_count, -1) * weights_half[:, :, None], axis=1)
        )
    return (after_mix + jnp.concatenate(pieces, axis=0)).astype(jnp.bfloat16)


def solution(mesh):
    placed = (
        P(("sp", "tp"), None),
        P("sp", "tp"),
        P("sp", "tp"),
        P("sp", "tp"),
        P(("sp", "tp"), None),
        P("tp", "sp"),
        P("tp", "sp"),
        P(),
        P(),
        P(),
        P(("sp", "tp"), None),
        P(("sp", "tp"), None),
        P("sp", None, None),
        P("sp", None, None),
        P("sp", None, None),
    )
    return jax.shard_map(
        shards, mesh=mesh, in_specs=placed, out_specs=P(("sp", "tp"), None), check_vma=False
    )
```
